512 devices in a mesh: ep: 32 (over z, x), tp: 16 (over y, core).
Axes of the slice: x: 4, y: 8, z: 8, core: 2. Of those that a mesh axis runs over, the one named last changes fastest.
Arguments:
- tokens: bfloat16 [1024, 2048], P(('ep', 'tp')), may hold values from -6 to 6
- cache_keys: bfloat16 [1024, 1024, 256], P(('ep', 'tp')), may hold values from -360 to 360
- cache_values: bfloat16 [1024, 1024, 256], P(('ep', 'tp')), may hold values from -6 to 6
- cache_gates: float32 [1024, 2, 1024], P(('ep', 'tp')), may hold values from -256 to 0, as said below
- lengths: int32 [1024], P(('ep', 'tp')), may hold values from 1 to 1024, 524288 in all
- routes: int32 [1024, 4], P(('ep', 'tp')), may hold values from 0 to 31, all different within a row; in each aligned block of 2 rows (0 to 1, 2 to 3, ...) no two rows name the same one
- route_logits: float32 [1024, 4], P(('ep', 'tp')), may hold values from -6 to 6
- attn_gain: float32 [2048], replicated, may hold values from 0.1 to 1.9
- w_query: bfloat16 [2048, 2048], P(None, 'tp'), may hold values from -0.125 to 0.125
- w_keyval: bfloat16 [2048, 512], P(None, 'tp'), may hold values from -0.125 to 0.125
- w_forget: bfloat16 [2048, 2], replicated, may hold values from -0.125 to 0.125
- forget_bias: float32 [2], replicated, may hold values from -1 to 3
- w_out: bfloat16 [2048, 2048], P(None, 'tp'), may hold values from -0.125 to 0.125
- mix_gain: float32 [2048], replicated, may hold values from 0.1 to 1.9
- ffn_gain: float32 [2048], replicated, may hold values from 0.1 to 1.9
- w_gate: bfloat16 [32, 2048, 2048], P('ep', None, 'tp'), may hold values from -0.125 to 0.125
- w_lin: bfloat16 [32, 2048, 2048], P('ep', None, 'tp'), may hold values from -0.125 to 0.125
- gate_bias: float32 [32, 2048], P('ep', 'tp'), may hold values from -12 to 12
- lin_bias: float32 [32, 2048], P('ep', 'tp'), may hold values from -12 to 12
- w_down: bfloat16 [32, 2048, 2048], P('ep', 'tp'), may hold values from -0.125 to 0.125
- post_gain: float32 [2048], replicated, may hold values from 0.1 to 1.9
Outputs:
- updated: bfloat16 [1024, 2048], P(('ep', 'tp'))
- new_entries: bfloat16 [1024, 512], P(('ep', 'tp'))
The draws below stay inside these ranges and needn't reach their ends.
Inputs may be any that keep to these rules, and one draw needn't show every extreme that they name: `cache_gates`: along the positions of each sequence and head the values never increase. The lengths of all sequences add up to 524288, and some sequence has exactly 1024. `routes`: each row names 4 different experts; among the rows of one device no expert is named twice; every expert is named by some row.
All inputs are finite; a program needn't handle non-finite values. No bound on the sum of `lengths` on one device may be relied on, other than what follows from the above.
Results may differ from the reference program's by a relative error of at most 0.014.
The reference program's roundings to bfloat16 on the way count: a program that leaves them out, or rounds other values in their place, can miss the bound.
Values may be sent and summed in bfloat16 or wider, within the bound.
A program may use at most 64 MiB of HBM per device.

```python
import math
import jax
import jax.numpy as jnp
import numpy as np
from jax import lax

D = 2048
HEADS = 16
KVH = 2
HDIM = 128
FF = 2048
TOPK = 4
SEQ_DEV = 2
LEN = 1024
TOKENS = 1024
EXPERTS = 32
N_TP = 16


def draw_cache_keys(key, part):
    first = jax.random.fold_in(jax.random.fold_in(key, 11), 0)
    values = jax.random.normal(first, (TOKENS, LEN, KVH * HDIM), jnp.float32)
    return jnp.clip(values, -360.0, 360.0).astype(jnp.bfloat16)


def draw_cache_gates(key, part):
    parts = jax.random.split(jax.random.fold_in(key, 23), 6)
    span = 32
    noise = jax.random.uniform(parts[0], (TOKENS, KVH, LEN), jnp.float32, 0.5, 1.5)
    blocks = jnp.exp(jax.random.uniform(parts[1], (TOKENS, 1, LEN // span), jnp.float32, -0.7, 0.7))
    blocks = jnp.repeat(blocks, span, axis=2)
    per_seq = jnp.exp(jax.random.uniform(parts[2], (TOKENS, 1, 1), jnp.float32, -0.7, 0.7))
    share = 0.5
    slow = jax.random.uniform(parts[3], (TOKENS, KVH, 1), jnp.float32) < share
    fast_rate = jnp.exp(jax.random.uniform(parts[4], (TOKENS, KVH, 1), jnp.float32, math.log(1.0 / 60.0), math.log(1.0 / 30.0)))
    slow_rate = jnp.exp(jax.random.uniform(parts[5], (TOKENS, KVH, 1), jnp.float32, -0.7, 0.0)) / LEN
    rate = jnp.where(slow, slow_rate, fast_rate)
    return jnp.cumsum(-rate * noise * blocks * per_seq, axis=2)


def block_levels(own_key, extent, cuts, smallest, largest):
    level, own = 1.0, jax.random.fold_in(own_key, 6)
    for axis_at, blocks in cuts:
        draws = jnp.exp(jax.random.uniform(jax.random.fold_in(own, axis_at), (blocks,), jnp.float32, smallest / len(cuts), largest / len(cuts)))
        level = level * jnp.repeat(draws, extent[axis_at] // blocks).reshape([-1 if axis == axis_at else 1 for axis in range(len(extent))])
    return level


def split_up(number_of, total, bound, lean):
    loads = [(1 << 20) // math.isqrt(grade ** lean) + 1 for grade in range(2, number_of + 1)]
    rest, counts = total - bound - (number_of - 1), [1] * (number_of - 1)
    while rest > 0:
        movable = [i for i in range(number_of - 1) if counts[i] < bound]
        whole, left = sum([loads[i] for i in movable]), rest
        for i in movable:
            addition = min(bound - counts[i], max(1, left * loads[i] // whole), rest)
            counts[i] = counts[i] + addition
            rest = rest - addition
    return np.array([bound] + counts)


def ragged(own_key, number_of, total, limit, skew):
    if number_of == 2:
        one = jax.random.randint(own_key, (), max(1, total - limit), min(limit, total - 1) + 1)
        return jnp.stack([one, total - one])
    sizes = jnp.asarray(split_up(number_of, total, limit, skew), jnp.int32)
    couples = (number_of - 1) // 2
    donor, receiver = sizes[1:1 + 2 * couples:2], sizes[2:2 + 2 * couples:2]
    slack = jnp.minimum(donor - 1, limit - receiver)
    moved = jax.random.randint(jax.random.fold_in(own_key, 1), (couples,), 0, 1 << 20) % (slack + 1)
    sizes = sizes.at[1:1 + 2 * couples:2].set(donor - moved).at[2:2 + 2 * couples:2].set(receiver + moved)
    return sizes[jax.random.permutation(jax.random.fold_in(own_key, 2), number_of)]


def routed_block(rng, own, number, rows, amount, top, reach, skew):
    ranking = jax.random.permutation(rng, amount)
    heavy_load, usual = load_shares(amount, rows * top, reach, skew, True), load_shares(amount, rows * top, reach, skew, False)
    places = jnp.arange(amount)

    def named(sizes, rotation):
        used = int((sizes > 0).sum())
        fixed = max(1, used // 4)
        passed = fixed + (places - fixed + rotation * (used - fixed)) % max(1, amount - fixed)
        return jnp.zeros((amount,), jnp.int32).at[ranking[jnp.where(places < fixed, places, passed)]].set(jnp.asarray(sizes, jnp.int32))

    sizes = jnp.where(number % 4 == 0, named(heavy_load, number // 4), named(usual, number - number // 4 - 1))
    mixed = jax.random.permutation(jax.random.fold_in(own, 3), amount)
    donor, sink = mixed[0:amount // 2 * 2:2], mixed[1:amount // 2 * 2:2]
    margin = jnp.minimum(sizes[donor] - 1, reach - sizes[sink]) // 2
    margin = jnp.where((donor == ranking[0]) | (sink == ranking[0]) | (sizes[sink] == 0), 0, jnp.maximum(margin, 0))
    passed = jax.random.randint(jax.random.fold_in(own, 4), (amount // 2,), 0, 1 << 20) % (margin + 1)
    sizes = sizes.at[donor].add(-passed).at[sink].add(passed)
    labels = jnp.searchsorted(jnp.cumsum(sizes), jnp.arange(rows * top), side="right").astype(jnp.int32)
    table = labels.reshape(top, rows).T
    table = table[jax.random.permutation(jax.random.fold_in(own, 1), rows)]
    rotation = jax.random.randint(jax.random.fold_in(own, 2), (rows, 1), 0, top)
    return jnp.take_along_axis(table, (jnp.arange(top)[None, :] + rotation) % top, axis=1)


def load_shares(amount, total, reach, skew, full):
    portions = [(1 << 20) // math.isqrt(grade ** skew) + 1 for grade in range(1, amount + 1)]
    largest = reach if full else min(reach, max(-(-total // amount), total * portions[0] // sum(portions)))
    least = 1 if total - largest >= amount - 1 else 0
    given, rest = [largest] + [least] * (amount - 1), total - largest - least * (amount - 1)
    while rest > 0:
        free = [i for i in range(1, amount) if given[i] < largest] or [i for i in range(1, amount) if given[i] < reach]
        whole, budget = sum([portions[i] for i in free]), rest
        for i in free:
            more = min(reach - given[i], max(1, budget * portions[i] // whole), rest)
            given[i] = given[i] + more
            rest = rest - more
    return np.array(given)


def gaussian(key, shape, deviation, reach, pieces=(), held_as=jnp.bfloat16):
    drawn = jax.random.normal(key, shape, jnp.float32) * deviation
    if len(pieces) > 0:
        drawn = block_levels(key, shape, pieces, -0.22, 0.18) * drawn
    return jnp.clip(drawn, min=-reach, max=reach).astype(held_as)


def setup_inputs(seed: int = 0) -> dict:
    splits = jax.random.split(jax.random.key(seed), 22)
    tokens = gaussian(splits[0], (TOKENS, D), 1.0, 6.0, ((0, 512),))
    cache_keys = draw_cache_keys(jax.random.fold_in(splits[21], 71), 0)
    cache_values = gaussian(splits[2], (TOKENS, LEN, KVH * HDIM), 1.0, 6.0, ((0, 512),))
    cache_gates = draw_cache_gates(jax.random.fold_in(splits[21], 71), 0)
    lengths = ragged(splits[4], TOKENS, TOKENS * LEN // 2, LEN, 2).astype(jnp.int32)
    routes_keys = jax.random.split(jax.random.fold_in(splits[5], 1), TOKENS // SEQ_DEV)
    routes_turns = jax.random.permutation(jax.random.fold_in(splits[5], 3), TOKENS // SEQ_DEV)
    routes = jax.vmap(lambda own, number: routed_block(jax.random.fold_in(splits[5], 2), own, number, SEQ_DEV, EXPERTS, TOPK, 1, 2))(routes_keys, routes_turns).reshape((TOKENS, TOPK))
    route_logits = gaussian(splits[6], (TOKENS, TOPK), 1.0, 6.0, ((0, 512),), jnp.float32)
    attn_gain = jnp.clip(1.0 + 0.18 * jax.random.normal(splits[7], (D,), jnp.float32), 0.1, 1.9)
    w_query = gaussian(splits[8], (D, HEADS * HDIM), D ** -0.5, 0.125, ((1, 16),))
    w_keyval = gaussian(splits[9], (D, 2 * KVH * HDIM), D ** -0.5, 0.125, ((1, 16),))
    w_forget = gaussian(splits[10], (D, KVH), D ** -0.5, 0.125)
    forget_bias = jnp.clip(jax.random.uniform(splits[11], (KVH,), jnp.float32, -1.0, 3.0), -1.0, 3.0)
    w_out = gaussian(splits[12], (HEADS * HDIM, D), (HEADS * HDIM) ** -0.5, 0.125, ((1, 16),))
    mix_gain = jnp.clip(1.0 + 0.18 * jax.random.normal(splits[13], (D,), jnp.float32), 0.1, 1.9)
    ffn_gain = jnp.clip(1.0 + 0.18 * jax.random.normal(splits[14], (D,), jnp.float32), 0.1, 1.9)
    w_gate = gaussian(splits[15], (EXPERTS, D, FF), D ** -0.5, 0.125, ((0, 32), (2, 16)))
    w_lin = gaussian(splits[16], (EXPERTS, D, FF), D ** -0.5, 0.125, ((0, 32), (2, 16)))
    gate_bias = gaussian(splits[17], (EXPERTS, FF), 3.0, 12.0, ((0, 32), (1, 16)), jnp.float32)
    lin_bias = gaussian(splits[18], (EXPERTS, FF), 3.0, 12.0, ((0, 32), (1, 16)), jnp.float32)
    w_down = gaussian(splits[19], (EXPERTS, FF, D), FF ** -0.5, 0.125, ((0, 32), (1, 16)))
    post_gain = jnp.clip(1.0 + 0.18 * jax.random.normal(splits[20], (D,), jnp.float32), 0.1, 1.9)
    return dict(tokens=tokens, cache_keys=cache_keys, cache_values=cache_values, cache_gates=cache_gates, lengths=lengths, routes=routes, route_logits=route_logits, attn_gain=attn_gain, w_query=w_query, w_keyval=w_keyval, w_forget=w_forget, forget_bias=forget_bias, w_out=w_out, mix_gain=mix_gain, ffn_gain=ffn_gain, w_gate=w_gate, w_lin=w_lin, gate_bias=gate_bias, lin_bias=lin_bias, w_down=w_down, post_gain=post_gain)


NORM_EPS = 1e-06
SWIGLU_ALPHA = 1.702
SWIGLU_LIMIT = 7.0
NEG_LARGE = -1e+30

def to_half(values):
    return lax.optimization_barrier(values.astype(jnp.bfloat16)).astype(jnp.float32)

def rms_scale(values, gain):
    values = values.astype(jnp.float32)
    return values * lax.rsqrt(lax.optimization_barrier(jnp.mean(values * values, axis=-1, keepdims=True)) + NORM_EPS) * gain.astype(jnp.float32)

def clamped_unit(gate, linear):
    gate = jnp.minimum(gate, SWIGLU_LIMIT)
    linear = jnp.clip(linear, -SWIGLU_LIMIT, SWIGLU_LIMIT)
    return gate * jax.nn.sigmoid(SWIGLU_ALPHA * gate) * (linear + 1.0)

def attend_one(args):
    query, fresh, keys, values, gates, length, forget = args
    group = HEADS // KVH
    q_four = query.reshape(KVH, group, HDIM).astype(jnp.float32)
    k_four = keys.reshape(LEN, KVH, HDIM).astype(jnp.float32)
    v_four = values.reshape(LEN, KVH, HDIM).astype(jnp.float32)
    new_key = fresh[:KVH * HDIM].reshape(KVH, HDIM).astype(jnp.float32)
    new_value = fresh[KVH * HDIM:].reshape(KVH, HDIM).astype(jnp.float32)
    place = jnp.arange(LEN, dtype=jnp.int32)
    last = lax.optimization_barrier(jnp.sum(jnp.where(place[None, :] == length - 1, gates, 0.0), axis=1))
    base = last + forget
    scale = HDIM ** (-0.5)
    scores = jnp.einsum('gqd,pgd->gqp', q_four, k_four) * scale + (base[:, None, None] - gates[:, None, :])
    live = place[None, None, :] < length
    masked = jnp.where(live, scores, NEG_LARGE)
    own = jnp.einsum('gqd,gd->gq', q_four, new_key) * scale
    top = jnp.maximum(lax.optimization_barrier(jnp.max(masked, axis=-1)), own)
    expo = jnp.where(live, jnp.exp(masked - top[..., None]), 0.0)
    own_expo = jnp.exp(own - top)
    total = lax.optimization_barrier(jnp.sum(expo, axis=-1)) + own_expo
    weights = to_half(expo / total[..., None])
    own_weight = to_half(own_expo / total)
    mixed = jnp.einsum('gqp,pgd->gqd', weights, v_four) + own_weight[..., None] * new_value[:, None, :]
    return mixed.reshape(HEADS * HDIM).astype(jnp.bfloat16)

def reference(tokens, cache_keys, cache_values, cache_gates, lengths, routes, route_logits, attn_gain, w_query, w_keyval, w_forget, forget_bias, w_out, mix_gain, ffn_gain, w_gate, w_lin, gate_bias, lin_bias, w_down, post_gain):
    normed = rms_scale(tokens, attn_gain).astype(jnp.bfloat16)
    query = jnp.dot(normed, w_query, preferred_element_type=jnp.float32).astype(jnp.bfloat16)
    fresh = jnp.dot(normed, w_keyval, preferred_element_type=jnp.float32).astype(jnp.bfloat16)
    forget = jax.nn.log_sigmoid(jnp.dot(normed, w_forget, preferred_element_type=jnp.float32) + forget_bias.astype(jnp.float32))
    mixed = lax.map(attend_one, (query, fresh, cache_keys, cache_values, cache_gates, lengths.astype(jnp.int32), forget))
    projected = jnp.dot(mixed, w_out, preferred_element_type=jnp.float32).astype(jnp.bfloat16)
    residual = tokens.astype(jnp.float32) + rms_scale(projected, mix_gain)
    expert_in = rms_scale(residual, ffn_gain).astype(jnp.bfloat16)
    hit = (routes[:, :, None] == jnp.arange(EXPERTS, dtype=jnp.int32)[None, None, :]).astype(jnp.float32)
    probs = jax.nn.softmax(route_logits.astype(jnp.float32), axis=-1)
    combine = lax.optimization_barrier(jnp.sum(probs[:, :, None] * hit, axis=1))

    def expert_step(total, items):
        gate_w, lin_w, gate_b, lin_b, down_w, share = items
        gate = jnp.dot(expert_in, gate_w, preferred_element_type=jnp.float32) + gate_b.astype(jnp.float32)
        linear = jnp.dot(expert_in, lin_w, preferred_element_type=jnp.float32) + lin_b.astype(jnp.float32)
        act = clamped_unit(gate, linear).astype(jnp.bfloat16)
        blocked = act.reshape(TOKENS, N_TP, FF // N_TP).astype(jnp.float32)
        down_blocks = down_w.reshape(N_TP, FF // N_TP, D).astype(jnp.float32)
        parts = to_half(jnp.einsum('tnf,nfd->ntd', blocked, down_blocks))
        expert_out = to_half(lax.optimization_barrier(jnp.sum(parts, axis=0)))
        return (total + share[:, None] * expert_out, None)
    moe, _ = lax.scan(expert_step, jnp.zeros((TOKENS, D), jnp.float32), (w_gate, w_lin, gate_bias, lin_bias, w_down, combine.T))
    updated = (residual + rms_scale(moe, post_gain)).astype(jnp.bfloat16)
    return (updated, fresh)
```

```python
import functools

import jax
import jax.numpy as jnp
from jax import lax
from jax.experimental import pallas as pl
from jax.experimental.pallas import tpu as pltpu
from jax.sharding import PartitionSpec as P

HEADS = 16
KVH = 2
HDIM = 128

NORM_EPS = 1e-06
SWIGLU_ALPHA = 1.702
SWIGLU_LIMIT = 7.0
NEG_LARGE = -1e30
MESH = pl.DeviceIdType.MESH
CORES = 2
F32 = jnp.float32
BF16 = jnp.bfloat16


def laid_out(tiles, dim):
    shape = list(tiles.shape[1:])
    shape[dim] *= tiles.shape[0]
    return jnp.moveaxis(tiles, 0, dim).reshape(shape)


def sent_to_all(array, axis):
    copies = jnp.broadcast_to(array, (lax.axis_size(axis), *array.shape))
    return lax.all_to_all(copies, axis, split_axis=0, concat_axis=0, tiled=True)


def gather_directly(array, axis, dim):
    return laid_out(sent_to_all(array, axis), dim)


def rms_scale(values, gain):
    values = values.astype(F32)
    return values * lax.rsqrt(jnp.mean(values * values, axis=-1, keepdims=True) + NORM_EPS) * gain


def clamped_unit(gate, linear):
    gate = jnp.minimum(gate, SWIGLU_LIMIT)
    linear = jnp.clip(linear, -SWIGLU_LIMIT, SWIGLU_LIMIT)
    return gate * jax.nn.sigmoid(SWIGLU_ALPHA * gate) * (linear + 1.0)


def goes(way, chunk, reach, half):
    return 1 <= reach <= (half if way == chunk else half - 1)


def remote(src, dst, send_sem, recv_sem, to):
    return pltpu.make_async_remote_copy(
        src_ref=src, dst_ref=dst, send_sem=send_sem, recv_sem=recv_sem,
        device_id=to, device_id_type=MESH,
    )


def arrived(ref, sem):
    pltpu.make_async_copy(ref, ref, sem).wait()


def split_rows(row):
    half = row.shape[1] // 2
    return jnp.concatenate([row[:, :half], row[:, half:]], axis=0)


def expert_kernel(
    residual_ref, ffn_gain_ref, post_gain_ref, routes_ref, logits_ref, gate_bias_ref, lin_bias_ref,
    w_gate_hbm, w_lin_hbm, w_down_hbm,
    out_ref,
    w_in, w_down, outbox, inbox, rows, parts, peer_parts, ring_in, ring_out, back_out, back_in,
    load_sem, go_send, go_recv, self_sem, cw_send, ccw_send, core_send, ring_recv, core_recv,
    part_send, part_recv, sum_send, sum_recv, back_send, back_recv,
):
    eps = lax.axis_size("ep")
    tps = lax.axis_size("tp")
    ny = tps // CORES
    half = ny // 2
    seqs, width = residual_ref.shape
    hidden = w_down.shape[0]
    chunk_rows = eps // 2
    me_ep = lax.axis_index("ep")
    me_tp = lax.axis_index("tp")
    me_y = me_tp // CORES
    me_c = me_tp % CORES

    def at(shift, core=None):
        core = me_c if core is None else core
        return {"tp": lax.rem(me_y + shift + ny, ny) * CORES + core}

    partner = at(0, 1 - me_c)

    loads = [
        pltpu.make_async_copy(w_gate_hbm.at[0], w_in.at[:, pl.ds(0, hidden)], load_sem.at[0]),
        pltpu.make_async_copy(w_lin_hbm.at[0], w_in.at[:, pl.ds(hidden, hidden)], load_sem.at[1]),
        pltpu.make_async_copy(w_down_hbm.at[0], w_down, load_sem.at[2]),
    ]
    for load in loads:
        load.start()

    barrier = pltpu.get_barrier_semaphore()
    near = [at(1), partner] + ([at(-1)] if ny > 2 else [])
    for to in near:
        pl.semaphore_signal(barrier, inc=1, device_id=to, device_id_type=MESH)
    far_first = sorted(range(1, eps), key=lambda d: -min(d, eps - d))
    for d in far_first:
        to = {"ep": lax.rem(me_ep + d, eps)}
        pl.semaphore_signal(barrier, inc=1, device_id=to, device_id_type=MESH)

    residual = residual_ref[...]
    expert_in = rms_scale(residual, ffn_gain_ref[...]).astype(BF16).astype(F32)
    routes = routes_ref[...]
    top = routes.shape[1]
    entry = lax.broadcasted_iota(jnp.int32, (2 * eps, 1), 0)
    owner, side = entry // 2, entry % 2
    hw = width // 2
    mail = jnp.zeros((2 * eps, hw), F32)
    for s in range(seqs):
        named = functools.reduce(
            jnp.logical_or, [owner == routes[s : s + 1, k : k + 1] for k in range(top)]
        )
        row = expert_in[s : s + 1, :]
        mail = jnp.where(named & (side == 0), row[:, :hw], mail)
        mail = jnp.where(named & (side == 1), row[:, hw:], mail)
    for e in range(eps):
        outbox[e] = mail[2 * e : 2 * e + 2, :].astype(BF16)

    pl.semaphore_wait(barrier, len(near) + eps - 1)
    for d in far_first:
        to = lax.rem(me_ep + d, eps)
        remote(
            outbox.at[to], inbox.at[me_ep], go_send, go_recv.at[me_ep // chunk_rows], {"ep": to}
        ).start()
    pltpu.make_async_copy(
        outbox.at[me_ep], inbox.at[me_ep], go_recv.at[me_ep // chunk_rows]
    ).start()

    probs = jax.nn.softmax(logits_ref[...], axis=-1)
    lane = lax.broadcasted_iota(jnp.int32, (seqs, eps), 1)
    combine = jnp.zeros((seqs, eps), F32)
    for k in range(top):
        combine += jnp.where(routes[:, k : k + 1] == lane, probs[:, k : k + 1], 0.0)

    def shift_of(slot):
        if slot == 0:
            return 0
        return -slot if slot <= half else slot - half

    def chip(slot):
        return lax.rem(me_y + shift_of(slot) + ny, ny)

    sends = []

    def pass_on(slot, g):
        block = rows.at[chip(slot), me_c, g]
        if slot == 0:
            ways = [(0, 1), (1, 1)]
        else:
            ways = [(0, slot + 1)] if slot <= half else [(1, slot - half + 1)]
        for way, reach in ways:
            if goes(way, g, reach, half):
                there = reach if way == 0 else half + reach
                sends.append(remote(
                    block, block, (cw_send if way == 0 else ccw_send).at[slot, g],
                    ring_recv.at[there, g], at(1 if way == 0 else -1),
                ))
                sends[-1].start()
        sends.append(remote(block, block, core_send.at[slot, g], core_recv.at[slot, g], partner))
        sends[-1].start()

    for g in range(2):
        first = g * chunk_rows
        arrived(inbox.at[pl.ds(first, chunk_rows)], go_recv.at[g])
        pairs = [inbox[first + i].astype(F32) for i in range(chunk_rows)]
        rows[me_y, me_c, g] = jnp.concatenate(
            [
                jnp.concatenate([pair[0:1] for pair in pairs], axis=0),
                jnp.concatenate([pair[1:2] for pair in pairs], axis=0),
            ],
            axis=1,
        ).astype(BF16)
        pass_on(0, g)

    def slots_at(reach):
        if reach == 0:
            return [(0, (0, 1))]
        found = []
        for way in range(2):
            gs = tuple(g for g in range(2) if goes(way, g, reach, half))
            if gs:
                found.append((reach if way == 0 else half + reach, gs))
        return found

    def work(reach):
        slots = slots_at(reach)
        for slot, gs in slots:
            for g in gs:
                block = rows.at[chip(slot), 1 - me_c, g]
                arrived(block, core_recv.at[slot, g])
        for slot in [slots[0][0]] if reach == half else [slot for slot, _ in slots]:
            place = chip(slot)
            x = rows[place].reshape(4 * chunk_rows, width)
            both = jnp.dot(x, w_in[...], preferred_element_type=F32)
            act = clamped_unit(
                both[:, :hidden] + gate_bias_ref[...], both[:, hidden:] + lin_bias_ref[...]
            ).astype(BF16)
            out = jnp.dot(act, w_down[...], preferred_element_type=F32).astype(BF16)
            parts[place] = out.reshape(2, 2, chunk_rows, width)
            sends.append(remote(
                parts.at[place, 1 - me_c], peer_parts.at[place], part_send.at[slot],
                part_recv.at[slot], partner,
            ))
            sends[-1].start()

    for load in loads:
        load.wait()
    for reach in range(1, half + 1):
        for slot, gs in sorted(slots_at(reach), key=lambda pair: pair[1]):
            for g in gs:
                arrived(rows.at[chip(slot), me_c, g], ring_recv.at[slot, g])
                pass_on(slot, g)
        work(reach - 1)
    work(half)

    seen = set()

    def local_sum(slot, g):
        place = chip(slot)
        if slot not in seen:
            arrived(peer_parts.at[place], part_recv.at[slot])
            seen.add(slot)
        return parts[place, me_c, g].astype(F32) + peer_parts[place, g].astype(F32)

    def inward(way, reach, g):
        arrived(ring_in.at[way, reach, g], sum_recv.at[way, reach, g])
        return ring_in[way, reach, g].astype(F32)

    for reach in range(half, 0, -1):
        for way, g in [(0, 1), (1, 0), (0, 0), (1, 1)]:
            if not goes(way, g, reach, half):
                continue
            slot = half if reach == half else (half + reach if way == 0 else reach)
            total = local_sum(slot, g)
            if goes(way, g, reach + 1, half):
                total += inward(way, reach + 1, g)
            ring_out[way, reach, g] = total.astype(BF16)
            sends.append(remote(
                ring_out.at[way, reach, g], ring_in.at[way, reach, g],
                sum_send.at[way, reach, g], sum_recv.at[way, reach, g],
                at(1 if way == 0 else -1),
            ))
            sends[-1].start()

    for g in range(2):
        total = local_sum(0, g)
        for way in range(2):
            if goes(way, g, 1, half):
                total += inward(way, 1, g)
        for i in range(chunk_rows):
            back_out[g * chunk_rows + i] = split_rows(total[i : i + 1, :]).astype(BF16)
        for i in range(chunk_rows):
            to = g * chunk_rows + i

            @pl.when(me_ep != to)
            def _():
                remote(
                    back_out.at[to], back_in.at[me_ep], back_send, back_recv, {"ep": to}
                ).start()

            @pl.when(me_ep == to)
            def _():
                pltpu.make_async_copy(back_out.at[to], back_in.at[me_ep], back_recv).start()

    arrived(back_in, back_recv)
    for s in range(seqs):
        moe = jnp.zeros((2, hw), F32)
        for e in range(eps):
            moe += combine[s : s + 1, e : e + 1] * back_in[e].astype(F32)
        mean = jnp.sum(jnp.sum(moe * moe, axis=1, keepdims=True), axis=0, keepdims=True) / width
        moe = moe * lax.rsqrt(mean + NORM_EPS) * split_rows(post_gain_ref[...])
        moe = jnp.concatenate([moe[0:1], moe[1:2]], axis=1)
        back_sum = residual[s : s + 1, :] + moe
        out_ref[s : s + 1, :] = back_sum

    for send in sends:
        send.wait_send()
    arrived(outbox.at[pl.ds(0, eps - 1)], go_send)
    arrived(back_out.at[pl.ds(0, eps - 1)], back_send)


def run_experts(residual, ffn_gain, post_gain, routes, logits, gate_bias, lin_bias, w_gate, w_lin, w_down):
    eps = lax.axis_size("ep")
    ny = lax.axis_size("tp") // CORES
    half = ny // 2
    seqs, width = residual.shape
    hidden = w_down.shape[1]
    r = eps // 2
    vmem = pl.BlockSpec(memory_space=pltpu.VMEM)
    anyspace = pl.BlockSpec(memory_space=pl.ANY)
    dma = pltpu.SemaphoreType.DMA
    slots = 2 * half + 1
    return pl.pallas_call(
        expert_kernel,
        out_shape=jax.ShapeDtypeStruct((seqs, width), F32),
        in_specs=[vmem] * 7 + [anyspace] * 3,
        out_specs=vmem,
        scratch_shapes=[
            pltpu.VMEM((width, 2 * hidden), BF16),
            pltpu.VMEM((hidden, width), BF16),
            pltpu.VMEM((eps, 2, width // 2), BF16),
            pltpu.VMEM((eps, 2, width // 2), BF16),
            pltpu.VMEM((ny, 2, 2, r, width), BF16),
            pltpu.VMEM((ny, 2, 2, r, width), BF16),
            pltpu.VMEM((ny, 2, r, width), BF16),
            pltpu.VMEM((2, half + 1, 2, r, width), BF16),
            pltpu.VMEM((2, half + 1, 2, r, width), BF16),
            pltpu.VMEM((eps, 2, width // 2), BF16),
            pltpu.VMEM((eps, 2, width // 2), BF16),
            dma((3,)),
            dma,
            dma((2,)),
            dma,
            dma((slots, 2)),
            dma((slots, 2)),
            dma((slots, 2)),
            dma((slots, 2)),
            dma((slots, 2)),
            dma((slots,)),
            dma((slots,)),
            dma((2, half + 1, 2)),
            dma((2, half + 1, 2)),
            dma,
            dma,
        ],
        compiler_params=pltpu.CompilerParams(
            collective_id=0, has_side_effects=True, vmem_limit_bytes=40 * 1024 * 1024
        ),
        name="experts",
    )(residual, ffn_gain, post_gain, routes, logits, gate_bias, lin_bias, w_gate, w_lin, w_down)


def block_scores(q_four, cache_keys, cache_gates, base, lengths, span, scale):
    seqs = cache_keys.shape[0]
    k_four = cache_keys.reshape(seqs, span, q_four.shape[1], q_four.shape[3])
    scores = (
        jnp.einsum("sgqd,spgd->sgqp", q_four, k_four, preferred_element_type=jnp.float32) * scale
    )
    scores = scores + (base[:, :, None, None] - cache_gates[:, :, None, :])
    place = lax.iota(jnp.int32, span)
    live = place[None, None, None, :] < lengths[:, None, None, None]
    return (jnp.where(live, scores, NEG_LARGE), live)


def per_device(
    tokens,
    cache_keys,
    cache_values,
    cache_gates,
    lengths,
    routes,
    route_logits,
    attn_gain,
    w_query,
    w_keyval,
    w_forget,
    forget_bias,
    w_out,
    mix_gain,
    ffn_gain,
    w_gate,
    w_lin,
    gate_bias,
    lin_bias,
    w_down,
    post_gain,
):
    seqs, width = tokens.shape
    normed = rms_scale(tokens, attn_gain).astype(jnp.bfloat16)
    query_cols = w_query.shape[1]
    pair_cols = w_keyval.shape[1]
    piece = gather_directly(normed, "tp", 0)
    both = jnp.concatenate(
        [
            jnp.dot(piece, w_query, preferred_element_type=jnp.float32),
            jnp.dot(piece, w_keyval, preferred_element_type=jnp.float32),
        ],
        axis=1,
    )
    gathered = both.astype(jnp.bfloat16)
    owned = lax.all_to_all(gathered, "tp", split_axis=0, concat_axis=1, tiled=True)
    groups = lax.axis_size("tp")
    owned = owned.reshape(seqs, groups, query_cols + pair_cols)
    query = owned[:, :, :query_cols].reshape(seqs, groups * query_cols)
    fresh = owned[:, :, query_cols:].reshape(seqs, groups * pair_cols)
    forget = jax.nn.log_sigmoid(
        jnp.dot(normed, w_forget, preferred_element_type=jnp.float32) + forget_bias
    )
    q_four = query.reshape(seqs, KVH, HEADS // KVH, HDIM)
    new_key = fresh[:, : KVH * HDIM].reshape(seqs, KVH, HDIM)
    new_value = fresh[:, KVH * HDIM :].reshape(seqs, KVH, HDIM)
    span_all = cache_keys.shape[1]
    place = lax.iota(jnp.int32, span_all)
    last = jnp.sum(
        jnp.where(place[None, None, :] == lengths[:, None, None] - 1, cache_gates, 0.0), axis=2
    )
    base = last + forget
    scale = HDIM ** (-0.5)
    own = jnp.einsum("sgqd,sgd->sgq", q_four, new_key, preferred_element_type=jnp.float32) * scale
    values_four = cache_values.reshape(seqs, span_all, KVH, HDIM)
    masked, live = block_scores(q_four, cache_keys, cache_gates, base, lengths, span_all, scale)
    top = jnp.maximum(jnp.max(masked, axis=-1), own)
    expo = jnp.where(live, jnp.exp(masked - top[..., None]), 0.0)
    own_expo = jnp.exp(own - top)
    total = jnp.sum(expo, axis=-1) + own_expo
    weights = (expo / total[..., None]).astype(jnp.bfloat16)
    mixed = jnp.einsum("sgqp,spgd->sgqd", weights, values_four, preferred_element_type=jnp.float32)
    own_weight = (own_expo / total).astype(jnp.bfloat16)
    mixed = (
        mixed
        + own_weight.astype(jnp.float32)[..., None] * new_value.astype(jnp.float32)[:, :, None, :]
    )
    mixed = mixed.reshape(seqs, HEADS * HDIM).astype(jnp.bfloat16)
    projected = jnp.dot(
        gather_directly(mixed, "tp", 0), w_out, preferred_element_type=jnp.float32
    ).astype(jnp.bfloat16)
    projected = lax.all_to_all(projected, "tp", split_axis=0, concat_axis=1, tiled=True)
    residual = tokens.astype(jnp.float32) + rms_scale(projected, mix_gain)
    updated = run_experts(
        residual, ffn_gain[None, :], post_gain[None, :], routes, route_logits, gate_bias, lin_bias,
        w_gate, w_lin, w_down,
    )
    return (updated.astype(BF16), fresh)


def solution(mesh):
    in_specs = (
        P(("ep", "tp"), None),
        P(("ep", "tp"), None, None),
        P(("ep", "tp"), None, None),
        P(("ep", "tp"), None, None),
        P(("ep", "tp")),
        P(("ep", "tp"), None),
        P(("ep", "tp"), None),
        P(),
        P(None, "tp"),
        P(None, "tp"),
        P(),
        P(),
        P(None, "tp"),
        P(),
        P(),
        P("ep", None, "tp"),
        P("ep", None, "tp"),
        P("ep", "tp"),
        P("ep", "tp"),
        P("ep", "tp", None),
        P(),
    )
    out_specs = (P(("ep", "tp"), None), P(("ep", "tp"), None))
    return jax.shard_map(
        per_device, mesh=mesh, in_specs=in_specs, out_specs=out_specs, check_vma=False
    )
```

```python
import functools
from types import SimpleNamespace

import jax
import jax.numpy as jnp
from jax import lax
from jax.experimental import pallas as pl
from jax.experimental.pallas import tpu as pltpu
from jax.sharding import PartitionSpec as P

HEADS = 16
KVH = 2
HDIM = 128

NORM_EPS = 1e-06
SWIGLU_ALPHA = 1.702
SWIGLU_LIMIT = 7.0
NEG_LARGE = -1e30
MESH = pl.DeviceIdType.MESH
CORES = 2
F32 = jnp.float32
BF16 = jnp.bfloat16


def rms_scale(values, gain):
    values = values.astype(F32)
    return values * lax.rsqrt(jnp.mean(values * values, axis=-1, keepdims=True) + NORM_EPS) * gain


def clamped_unit(gate, linear):
    gate = jnp.minimum(gate, SWIGLU_LIMIT)
    linear = jnp.clip(linear, -SWIGLU_LIMIT, SWIGLU_LIMIT)
    return gate * jax.nn.sigmoid(SWIGLU_ALPHA * gate) * (linear + 1.0)


def goes(way, chunk, reach, half):
    return 1 <= reach <= (half if way == chunk else half - 1)


def remote(src, dst, send_sem, recv_sem, to):
    return pltpu.make_async_remote_copy(
        src_ref=src, dst_ref=dst, send_sem=send_sem, recv_sem=recv_sem,
        device_id=to, device_id_type=MESH,
    )


def arrived(ref, sem):
    pltpu.make_async_copy(ref, ref, sem).wait()


def split_rows(row):
    half = row.shape[1] // 2
    return jnp.concatenate([row[:, :half], row[:, half:]], axis=0)


INPUTS = (
    "tokens", "lengths", "routes", "logits", "attn_gain", "forget_bias", "w_forget", "mix_gain",
    "ffn_gain", "post_gain", "gate_bias", "lin_bias", "keys_hbm", "values_hbm", "gates_hbm",
    "w_query_hbm", "w_keyval_hbm", "w_out_hbm", "w_gate_hbm", "w_lin_hbm", "w_down_hbm",
)
OUTPUTS = ("updated", "fresh")
SCRATCH = (
    "keys", "values", "gates", "w_query", "w_keyval", "w_out", "w_in", "w_down",
    "normed_out", "normed_in", "qkv_out", "qkv_in", "mixed_rows", "mixed_out", "mixed_in",
    "proj_out", "proj_in",
    "outbox", "inbox", "rows", "parts", "peer_parts", "ring_in", "ring_out", "back_out", "back_in",
    "load_sem", "normed_send", "normed_recv", "qkv_send", "qkv_recv", "mixed_send", "mixed_recv",
    "proj_send", "proj_recv",
    "go_send", "go_recv", "cw_send", "ccw_send", "core_send", "ring_recv", "core_recv",
    "part_send", "part_recv", "sum_send", "sum_recv", "back_send", "back_recv",
)


def layer_kernel(*refs):
    r = SimpleNamespace(**dict(zip(INPUTS + OUTPUTS + SCRATCH, refs, strict=True)))
    eps = lax.axis_size("ep")
    tps = lax.axis_size("tp")
    ny = tps // CORES
    half = ny // 2
    seqs, width = r.tokens.shape
    hidden = r.w_down.shape[0]
    chunk_rows = eps // 2
    me_ep = lax.axis_index("ep")
    me_tp = lax.axis_index("tp")
    me_y = me_tp // CORES
    me_c = me_tp % CORES

    def at(shift, core=None):
        core = me_c if core is None else core
        return {"tp": lax.rem(me_y + shift + ny, ny) * CORES + core}

    partner = at(0, 1 - me_c)

    pairs_to_load = {
        "query": (r.w_query_hbm, r.w_query),
        "keyval": (r.w_keyval_hbm, r.w_keyval),
        "keys": (r.keys_hbm, r.keys),
        "gates": (r.gates_hbm, r.gates),
        "values": (r.values_hbm, r.values),
        "out": (r.w_out_hbm, r.w_out),
        "gate": (r.w_gate_hbm.at[0], r.w_in.at[:, pl.ds(0, hidden)]),
        "lin": (r.w_lin_hbm.at[0], r.w_in.at[:, pl.ds(hidden, hidden)]),
        "down": (r.w_down_hbm.at[0], r.w_down),
    }

    barrier = pltpu.get_barrier_semaphore()
    far_first = sorted(range(1, eps), key=lambda d: -min(d, eps - d))
    peers = [
        (shift, core)
        for shift in sorted(range(ny), key=lambda d: -min(d, ny - d))
        for core in ((0, 1) if shift else (1,))
    ]

    def peer(shift, core):
        return lax.rem(me_y + shift, ny) * CORES + lax.rem(me_c + core, CORES)

    for d in far_first:
        to = {"ep": lax.rem(me_ep + d, eps)}
        pl.semaphore_signal(barrier, inc=1, device_id=to, device_id_type=MESH)
    for shift, core in peers:
        to = {"tp": peer(shift, core)}
        pl.semaphore_signal(barrier, inc=1, device_id=to, device_id_type=MESH)

    loads = {
        name: pltpu.make_async_copy(src, dst, r.load_sem.at[i])
        for i, (name, (src, dst)) in enumerate(pairs_to_load.items())
    }
    for load in loads.values():
        load.start()

    tokens = r.tokens[...].astype(F32)
    normed = rms_scale(tokens, r.attn_gain[...]).astype(BF16)
    r.normed_out[...] = normed

    pl.semaphore_wait(barrier, eps - 1 + tps - 1)

    def to_group(outbox_of, inbox, send, recv):
        for shift, core in peers:
            to = peer(shift, core)
            remote(outbox_of(to), inbox.at[me_tp], send, recv, {"tp": to}).start()
        pltpu.make_async_copy(outbox_of(me_tp), inbox.at[me_tp], recv).start()

    to_group(lambda to: r.normed_out, r.normed_in, r.normed_send, r.normed_recv)
    forget = jnp.concatenate(
        [
            jnp.sum(normed.astype(F32) * r.w_forget[g : g + 1, :].astype(F32), axis=1, keepdims=True)
            for g in range(KVH)
        ],
        axis=1,
    ) + r.forget_bias[...]
    forget = jnp.minimum(forget, 0.0) - jnp.log1p(jnp.exp(-jnp.abs(forget)))

    loads["query"].wait()
    loads["keyval"].wait()
    arrived(r.normed_in, r.normed_recv)
    piece = jnp.concatenate([r.normed_in[i].astype(F32) for i in range(tps)], axis=0).astype(BF16)
    query = jnp.dot(piece, r.w_query[...], preferred_element_type=F32)
    keyval = lax.dot_general(
        piece, r.w_keyval[...], (((1,), (1,)), ((), ())), preferred_element_type=F32
    )
    pair_cols = keyval.shape[1]
    both = jnp.concatenate(
        [query, keyval, jnp.zeros((seqs * tps, HDIM - pair_cols), F32)], axis=1
    )
    for i in range(tps):
        r.qkv_out[i] = both[seqs * i : seqs * (i + 1), :].astype(BF16)
    to_group(lambda to: r.qkv_out.at[to], r.qkv_in, r.qkv_send, r.qkv_recv)

    group = HEADS // KVH
    span = r.keys.shape[1]
    scale = HDIM ** (-0.5)
    head = lax.broadcasted_iota(jnp.int32, (HEADS, 1), 0)
    lower = head < group
    place = lax.broadcasted_iota(jnp.int32, (HEADS, span), 1)
    loads["keys"].wait()
    loads["gates"].wait()
    loads["values"].wait()
    arrived(r.qkv_in, r.qkv_recv)
    per_tile = HDIM // pair_cols
    fresh_rows = []
    for s in range(seqs):
        mine = jnp.concatenate([r.qkv_in[j].astype(F32)[s : s + 1, :] for j in range(tps)], axis=0)
        q = mine[:, :HDIM]
        kv = mine[:, HDIM:]
        spread = kv
        for i in range(1, per_tile):
            spread = jnp.where(head % per_tile == i, pltpu.roll(kv, i * pair_cols, 1), spread)
        tiles = [
            jnp.sum(spread[per_tile * b : per_tile * (b + 1), :], axis=0, keepdims=True)
            for b in range(2 * KVH)
        ]
        fresh_rows.append(jnp.concatenate(tiles, axis=1))
        new_key = jnp.where(lower, tiles[0], tiles[1])
        new_value = jnp.where(lower, tiles[2], tiles[3])
        gates = jnp.where(lower, r.gates[s, 0:1, :], r.gates[s, 1:2, :])
        length = r.lengths[s]
        last = jnp.sum(jnp.where(place == length - 1, gates, 0.0), axis=1, keepdims=True)
        base = last + jnp.where(lower, forget[s : s + 1, 0:1], forget[s : s + 1, 1:2])
        own = jnp.sum(q * new_key, axis=1, keepdims=True) * scale
        q_wide = jnp.concatenate([jnp.where(lower, q, 0.0), jnp.where(lower, 0.0, q)], axis=1)
        score = lax.dot_general(
            q_wide.astype(BF16), r.keys[s], (((1,), (1,)), ((), ())), preferred_element_type=F32
        )
        live = place < length
        masked = jnp.where(live, score * scale + (base - gates), NEG_LARGE)
        top = jnp.maximum(jnp.max(masked, axis=1, keepdims=True), own)
        expo = jnp.where(live, jnp.exp(masked - top), 0.0)
        own_expo = jnp.exp(own - top)
        total = jnp.sum(expo, axis=1, keepdims=True) + own_expo
        weights = (expo / total).astype(BF16)
        own_weight = (own_expo / total).astype(BF16).astype(F32)
        mixed = jnp.dot(weights, r.values[s], preferred_element_type=F32)
        mixed = jnp.where(lower, mixed[:, :HDIM], mixed[:, HDIM:]) + own_weight * new_value
        for h in range(HEADS):
            r.mixed_rows[s : s + 1, h * HDIM : (h + 1) * HDIM] = mixed[h : h + 1, :]
    r.mixed_out[...] = r.mixed_rows[...].astype(BF16)
    to_group(lambda to: r.mixed_out, r.mixed_in, r.mixed_send, r.mixed_recv)
    r.fresh[...] = jnp.concatenate(fresh_rows, axis=0).astype(BF16)

    loads["out"].wait()
    arrived(r.mixed_in, r.mixed_recv)
    piece = jnp.concatenate([r.mixed_in[i].astype(F32) for i in range(tps)], axis=0).astype(BF16)
    projected = jnp.dot(piece, r.w_out[...], preferred_element_type=F32)
    for i in range(tps):
        r.proj_out[i] = projected[seqs * i : seqs * (i + 1), :].astype(BF16)
    to_group(lambda to: r.proj_out.at[to], r.proj_in, r.proj_send, r.proj_recv)
    arrived(r.proj_in, r.proj_recv)
    projected = jnp.concatenate([r.proj_in[j].astype(F32) for j in range(tps)], axis=1)
    residual = tokens + rms_scale(projected, r.mix_gain[...])

    expert_in = rms_scale(residual, r.ffn_gain[...]).astype(BF16).astype(F32)
    routes = r.routes[...]
    top = routes.shape[1]
    entry = lax.broadcasted_iota(jnp.int32, (2 * eps, 1), 0)
    owner, side = entry // 2, entry % 2
    hw = width // 2
    mail = jnp.zeros((2 * eps, hw), F32)
    for s in range(seqs):
        named = functools.reduce(
            jnp.logical_or, [owner == routes[s : s + 1, k : k + 1] for k in range(top)]
        )
        row = expert_in[s : s + 1, :]
        mail = jnp.where(named & (side == 0), row[:, :hw], mail)
        mail = jnp.where(named & (side == 1), row[:, hw:], mail)
    for e in range(eps):
        r.outbox[e] = mail[2 * e : 2 * e + 2, :].astype(BF16)

    for d in far_first:
        to = lax.rem(me_ep + d, eps)
        remote(
            r.outbox.at[to], r.inbox.at[me_ep], r.go_send, r.go_recv.at[me_ep // chunk_rows], {"ep": to}
        ).start()
    pltpu.make_async_copy(
        r.outbox.at[me_ep], r.inbox.at[me_ep], r.go_recv.at[me_ep // chunk_rows]
    ).start()

    probs = jax.nn.softmax(r.logits[...], axis=-1)
    lane = lax.broadcasted_iota(jnp.int32, (seqs, eps), 1)
    combine = jnp.zeros((seqs, eps), F32)
    for k in range(top):
        combine += jnp.where(routes[:, k : k + 1] == lane, probs[:, k : k + 1], 0.0)

    def shift_of(slot):
        if slot == 0:
            return 0
        return -slot if slot <= half else slot - half

    def chip(slot):
        return lax.rem(me_y + shift_of(slot) + ny, ny)

    sends = []

    def pass_on(slot, g):
        block = r.rows.at[chip(slot), me_c, g]
        if slot == 0:
            ways = [(0, 1), (1, 1)]
        else:
            ways = [(0, slot + 1)] if slot <= half else [(1, slot - half + 1)]
        for way, reach in ways:
            if goes(way, g, reach, half):
                there = reach if way == 0 else half + reach
                sends.append(remote(
                    block, block, (r.cw_send if way == 0 else r.ccw_send).at[slot, g],
                    r.ring_recv.at[there, g], at(1 if way == 0 else -1),
                ))
                sends[-1].start()
        sends.append(remote(block, block, r.core_send.at[slot, g], r.core_recv.at[slot, g], partner))
        sends[-1].start()

    for g in range(2):
        first = g * chunk_rows
        arrived(r.inbox.at[pl.ds(first, chunk_rows)], r.go_recv.at[g])
        pairs = [r.inbox[first + i].astype(F32) for i in range(chunk_rows)]
        r.rows[me_y, me_c, g] = jnp.concatenate(
            [
                jnp.concatenate([pair[0:1] for pair in pairs], axis=0),
                jnp.concatenate([pair[1:2] for pair in pairs], axis=0),
            ],
            axis=1,
        ).astype(BF16)
        pass_on(0, g)

    def slots_at(reach):
        if reach == 0:
            return [(0, (0, 1))]
        found = []
        for way in range(2):
            gs = tuple(g for g in range(2) if goes(way, g, reach, half))
            if gs:
                found.append((reach if way == 0 else half + reach, gs))
        return found

    def work(reach):
        slots = slots_at(reach)
        for slot, gs in slots:
            for g in gs:
                block = r.rows.at[chip(slot), 1 - me_c, g]
                arrived(block, r.core_recv.at[slot, g])
        for slot in [slots[0][0]] if reach == half else [slot for slot, _ in slots]:
            place = chip(slot)
            x = r.rows[place].reshape(4 * chunk_rows, width)
            both = jnp.dot(x, r.w_in[...], preferred_element_type=F32)
            act = clamped_unit(
                both[:, :hidden] + r.gate_bias[...], both[:, hidden:] + r.lin_bias[...]
            ).astype(BF16)
            out = jnp.dot(act, r.w_down[...], preferred_element_type=F32).astype(BF16)
            r.parts[place] = out.reshape(2, 2, chunk_rows, width)
            sends.append(remote(
                r.parts.at[place, 1 - me_c], r.peer_parts.at[place], r.part_send.at[slot],
                r.part_recv.at[slot], partner,
            ))
            sends[-1].start()

    for name in ("gate", "lin", "down"):
        loads[name].wait()
    for reach in range(1, half + 1):
        for slot, gs in sorted(slots_at(reach), key=lambda pair: pair[1]):
            for g in gs:
                arrived(r.rows.at[chip(slot), me_c, g], r.ring_recv.at[slot, g])
                pass_on(slot, g)
        work(reach - 1)
    work(half)

    seen = set()

    def local_sum(slot, g):
        place = chip(slot)
        if slot not in seen:
            arrived(r.peer_parts.at[place], r.part_recv.at[slot])
            seen.add(slot)
        return r.parts[place, me_c, g].astype(F32) + r.peer_parts[place, g].astype(F32)

    def inward(way, reach, g):
        arrived(r.ring_in.at[way, reach, g], r.sum_recv.at[way, reach, g])
        return r.ring_in[way, reach, g].astype(F32)

    for reach in range(half, 0, -1):
        for way, g in [(0, 1), (1, 0), (0, 0), (1, 1)]:
            if not goes(way, g, reach, half):
                continue
            slot = half if reach == half else (half + reach if way == 0 else reach)
            total = local_sum(slot, g)
            if goes(way, g, reach + 1, half):
                total += inward(way, reach + 1, g)
            r.ring_out[way, reach, g] = total.astype(BF16)
            sends.append(remote(
                r.ring_out.at[way, reach, g], r.ring_in.at[way, reach, g],
                r.sum_send.at[way, reach, g], r.sum_recv.at[way, reach, g],
                at(1 if way == 0 else -1),
            ))
            sends[-1].start()

    for g in range(2):
        total = local_sum(0, g)
        for way in range(2):
            if goes(way, g, 1, half):
                total += inward(way, 1, g)
        for i in range(chunk_rows):
            r.back_out[g * chunk_rows + i] = split_rows(total[i : i + 1, :]).astype(BF16)
        for i in range(chunk_rows):
            to = g * chunk_rows + i

            @pl.when(me_ep != to)
            def _():
                remote(
                    r.back_out.at[to], r.back_in.at[me_ep], r.back_send, r.back_recv, {"ep": to}
                ).start()

            @pl.when(me_ep == to)
            def _():
                pltpu.make_async_copy(r.back_out.at[to], r.back_in.at[me_ep], r.back_recv).start()

    arrived(r.back_in, r.back_recv)
    finished = []
    for s in range(seqs):
        moe = jnp.zeros((2, hw), F32)
        for e in range(eps):
            moe += combine[s : s + 1, e : e + 1] * r.back_in[e].astype(F32)
        mean = jnp.sum(jnp.sum(moe * moe, axis=1, keepdims=True), axis=0, keepdims=True) / width
        moe = moe * lax.rsqrt(mean + NORM_EPS) * split_rows(r.post_gain[...])
        moe = jnp.concatenate([moe[0:1], moe[1:2]], axis=1)
        finished.append(residual[s : s + 1, :] + moe)
    r.updated[...] = jnp.concatenate(finished, axis=0).astype(BF16)

    for send in sends:
        send.wait_send()
    arrived(r.normed_in.at[pl.ds(0, tps - 1)], r.normed_send)
    arrived(r.mixed_in.at[pl.ds(0, tps - 1)], r.mixed_send)
    arrived(r.qkv_out.at[pl.ds(0, tps - 1)], r.qkv_send)
    arrived(r.proj_out.at[pl.ds(0, tps - 1)], r.proj_send)
    arrived(r.outbox.at[pl.ds(0, eps - 1)], r.go_send)
    arrived(r.back_out.at[pl.ds(0, eps - 1)], r.back_send)


def per_device(
    tokens, cache_keys, cache_values, cache_gates, lengths, routes, route_logits, attn_gain,
    w_query, w_keyval, w_forget, forget_bias, w_out, mix_gain, ffn_gain, w_gate, w_lin, gate_bias,
    lin_bias, w_down, post_gain,
):
    eps = lax.axis_size("ep")
    tps = lax.axis_size("tp")
    ny = tps // CORES
    half = ny // 2
    seqs, width = tokens.shape
    span = cache_keys.shape[1]
    hidden = w_down.shape[1]
    cols = w_query.shape[1]
    pair_cols = w_keyval.shape[1]
    r = eps // 2
    slots = 2 * half + 1
    vmem = pl.BlockSpec(memory_space=pltpu.VMEM)
    smem = pl.BlockSpec(memory_space=pltpu.SMEM)
    anyspace = pl.BlockSpec(memory_space=pl.ANY)
    dma = pltpu.SemaphoreType.DMA
    scratch = dict(
        keys=pltpu.VMEM(cache_keys.shape, BF16),
        values=pltpu.VMEM(cache_values.shape, BF16),
        gates=pltpu.VMEM(cache_gates.shape, F32),
        w_query=pltpu.VMEM((width, cols), BF16),
        w_keyval=pltpu.VMEM((pair_cols, width), BF16),
        w_out=pltpu.VMEM((width, cols), BF16),
        w_in=pltpu.VMEM((width, 2 * hidden), BF16),
        w_down=pltpu.VMEM((hidden, width), BF16),
        normed_out=pltpu.VMEM((seqs, width), BF16),
        normed_in=pltpu.VMEM((tps, seqs, width), BF16),
        qkv_out=pltpu.VMEM((tps, seqs, 2 * HDIM), BF16),
        qkv_in=pltpu.VMEM((tps, seqs, 2 * HDIM), BF16),
        mixed_rows=pltpu.VMEM((seqs, width), F32),
        mixed_out=pltpu.VMEM((seqs, width), BF16),
        mixed_in=pltpu.VMEM((tps, seqs, width), BF16),
        proj_out=pltpu.VMEM((tps, seqs, cols), BF16),
        proj_in=pltpu.VMEM((tps, seqs, cols), BF16),
        outbox=pltpu.VMEM((eps, 2, width // 2), BF16),
        inbox=pltpu.VMEM((eps, 2, width // 2), BF16),
        rows=pltpu.VMEM((ny, 2, 2, r, width), BF16),
        parts=pltpu.VMEM((ny, 2, 2, r, width), BF16),
        peer_parts=pltpu.VMEM((ny, 2, r, width), BF16),
        ring_in=pltpu.VMEM((2, half + 1, 2, r, width), BF16),
        ring_out=pltpu.VMEM((2, half + 1, 2, r, width), BF16),
        back_out=pltpu.VMEM((eps, 2, width // 2), BF16),
        back_in=pltpu.VMEM((eps, 2, width // 2), BF16),
        load_sem=dma((9,)),
        normed_send=dma, normed_recv=dma, qkv_send=dma, qkv_recv=dma,
        mixed_send=dma, mixed_recv=dma, proj_send=dma, proj_recv=dma,
        go_send=dma, go_recv=dma((2,)),
        cw_send=dma((slots, 2)), ccw_send=dma((slots, 2)), core_send=dma((slots, 2)),
        ring_recv=dma((slots, 2)), core_recv=dma((slots, 2)),
        part_send=dma((slots,)), part_recv=dma((slots,)),
        sum_send=dma((2, half + 1, 2)), sum_recv=dma((2, half + 1, 2)),
        back_send=dma, back_recv=dma,
    )
    operands = dict(
        tokens=tokens, lengths=lengths, routes=routes, logits=route_logits,
        attn_gain=attn_gain[None, :], forget_bias=forget_bias[None, :], w_forget=w_forget.T,
        mix_gain=mix_gain[None, :], ffn_gain=ffn_gain[None, :], post_gain=post_gain[None, :],
        gate_bias=gate_bias, lin_bias=lin_bias, keys_hbm=cache_keys, values_hbm=cache_values,
        gates_hbm=cache_gates, w_query_hbm=w_query, w_keyval_hbm=w_keyval.T, w_out_hbm=w_out,
        w_gate_hbm=w_gate, w_lin_hbm=w_lin, w_down_hbm=w_down,
    )
    spaces = [
        anyspace if name.endswith("_hbm") else smem if name == "lengths" else vmem
        for name in INPUTS
    ]
    return pl.pallas_call(
        layer_kernel,
        out_shape=(
            jax.ShapeDtypeStruct((seqs, width), BF16),
            jax.ShapeDtypeStruct((seqs, 2 * KVH * HDIM), BF16),
        ),
        in_specs=spaces,
        out_specs=(vmem, vmem),
        scratch_shapes=[scratch[name] for name in SCRATCH],
        compiler_params=pltpu.CompilerParams(
            collective_id=0, has_side_effects=True, vmem_limit_bytes=48 * 1024 * 1024
        ),
        name="layer",
    )(*[operands[name] for name in INPUTS])


def solution(mesh):
    in_specs = (
        P(("ep", "tp"), None),
        P(("ep", "tp"), None, None),
        P(("ep", "tp"), None, None),
        P(("ep", "tp"), None, None),
        P(("ep", "tp")),
        P(("ep", "tp"), None),
        P(("ep", "tp"), None),
        P(),
        P(None, "tp"),
        P(None, "tp"),
        P(),
        P(),
        P(None, "tp"),
        P(),
        P(),
        P("ep", None, "tp"),
        P("ep", None, "tp"),
        P("ep", "tp"),
        P("ep", "tp"),
        P("ep", "tp", None),
        P(),
    )
    out_specs = (P(("ep", "tp"), None), P(("ep", "tp"), None))
    return jax.shard_map(
        per_device, mesh=mesh, in_specs=in_specs, out_specs=out_specs, check_vma=False
    )
```
